32 devices in a mesh: sp: 4 (over z), fs: 4 (over y, x), tp: 2 (over core).
Axes of the slice: x: 2, y: 2, z: 4, core: 2. Of those that a mesh axis runs over, the one named last changes fastest.
Arguments:
- tokens: bfloat16 [2048, 2048], P(('fs', 'sp'), 'tp'), parts along dimension 0, may hold values from -6 to 6
- norm_gain: float32 [2048], replicated, may hold values from 0.1 to 1.9
- w_recept: bfloat16 [2048, 1024], P('sp', 'tp'), may hold values from -0.125 to 0.125
- w_key_a: bfloat16 [2048, 1024], P('sp', 'tp'), may hold values from -0.125 to 0.125
- w_value_a: bfloat16 [2048, 1024], P('sp', 'tp'), may hold values from -0.125 to 0.125
- w_gate_a: bfloat16 [2048, 1024], P('sp', 'tp'), may hold values from -0.125 to 0.125
- decay_down_weight: bfloat16 [2048, 64], replicated, may hold values from -0.125 to 0.125
- decay_up_weight: bfloat16 [64, 1024], P(None, 'tp'), may hold values from -0.75 to 0.75
- rate_down_weight: bfloat16 [2048, 64], replicated, may hold values from -0.125 to 0.125
- rate_up_weight: bfloat16 [64, 1024], P(None, 'tp'), may hold values from -0.75 to 0.75
- decay_base: float32 [1024], P('tp'), may hold values from -12 to -2.5
- rate_base: float32 [1024], P('tp'), may hold values from -12 to 1
- rate_shift: float32 [2048, 16], P(('fs', 'sp'), 'tp'), parts along dimension 0, may hold values from 0 to 1.39
- jolts: float32 [2048, 16], P(('fs', 'sp'), 'tp'), parts along dimension 0, may hold values from 0 to 0.69
- group_gain: float32 [1024], P('tp'), may hold values from 0.1 to 1.9
- w_query_b: bfloat16 [2048, 1024], P('sp', 'tp'), may hold values from -0.125 to 0.125
- w_key_b: bfloat16 [2048, 1024], P('sp', 'tp'), may hold values from -0.125 to 0.125
- w_value_b: bfloat16 [2048, 1024], P('sp', 'tp'), may hold values from -0.125 to 0.125
- w_gate_b: bfloat16 [2048, 1024], P('sp', 'tp'), may hold values from -0.125 to 0.125
- score_offset: float32 [8], P('tp'), may hold values from -12 to -1
- w_out_a: bfloat16 [1024, 2048], P('tp'), may hold values from -0.125 to 0.125
- w_out_b: bfloat16 [1024, 2048], P('tp'), may hold values from -0.125 to 0.125
Outputs:
- mixed: bfloat16 [2048, 2048], P(('fs', 'sp', 'tp')), parts along dimension 0
- row_log: float32 [2048, 8], P(('fs', 'sp'), 'tp'), parts along dimension 0
The draws below stay inside these ranges and needn't reach their ends.
There are 4 independent parts, one for each index of `fs`. The reference program is written for one: setup_inputs(seed, part) draws one part's arguments, and reference() takes and returns one part's arrays. A program takes and returns all parts, laid end to end along the dimension named above; an argument that names none is the same for every part. Nothing has to cross between parts.
All inputs are finite; a program needn't handle non-finite values.
Results may differ from the reference program's by a relative error of at most 0.02.
Values may be sent and summed in bfloat16 or wider, within the bound.
A program may use at most 64 MiB of HBM per device.

```python
import jax
import jax.numpy as jnp
from jax import lax

MODEL_WIDTH = 2048
HEADS_A = 16
HEAD_A = 64
LOW_RANK_WIDTH = 64
HEADS_B = 8
HEAD_B = 128
TOK_DEV = 128
DECAY_CHANNELS = 1024
WIDTH_B = 1024
SEQ = 512
N_SP = 4
N_TP = 2


def head_speed(key):
    fast_share = 0.5
    return jax.random.uniform(jax.random.fold_in(key, 11), (HEADS_A,)) < fast_share


def draw_decay_base(key, part):
    forget_fast = head_speed(key)
    slow_level = jnp.log(jnp.log(10.0) / (0.607 * SEQ)) - 2.5
    base_level = jnp.where(forget_fast, -3.0, slow_level)
    jitter = jax.random.uniform(jax.random.fold_in(key, 15), (HEADS_A, HEAD_A), minval=-0.5, maxval=0.5)
    return (base_level[:, None] + jitter).reshape(DECAY_CHANNELS).astype(jnp.float32)


def draw_rate_base(key, part):
    forget_fast = head_speed(key)
    slow_level = jnp.log(0.15 * HEAD_A / SEQ)
    jitter = jax.random.uniform(jax.random.fold_in(key, 16), (HEADS_A, HEAD_A), minval=-0.5, maxval=0.5)
    fast_values = jax.random.uniform(jax.random.fold_in(key, 17), (HEADS_A, HEAD_A), minval=-1.0, maxval=1.0)
    values = jnp.where(forget_fast[:, None], fast_values, slow_level + jitter)
    return values.reshape(DECAY_CHANNELS).astype(jnp.float32)


def draw_rate_shift(key, part):
    blocks = SEQ // TOK_DEV
    factor = jax.random.uniform(jax.random.fold_in(key, 12), (blocks, HEADS_A), minval=0.0, maxval=1.386)
    return jnp.repeat(factor, TOK_DEV, axis=0).astype(jnp.float32)


def draw_jolts(key, part):
    place_key, depth_key = jax.random.split(jax.random.fold_in(key, 13), 2)
    places = jax.random.randint(place_key, (3, HEADS_A), 0, SEQ)
    depths = jax.random.uniform(depth_key, (3, HEADS_A), minval=0.22, maxval=0.69)
    positions = jnp.arange(SEQ, dtype=jnp.int32)[:, None, None]
    return jnp.max(jnp.where(positions == places[None], depths[None], 0.0), axis=1).astype(jnp.float32)


def draw_score_offset(key, part):
    far_end = -jnp.log(1.0 * SEQ) - 0.5
    offsets = jax.random.uniform(jax.random.fold_in(key, 14), (HEADS_B,), minval=far_end, maxval=-1.0)
    return offsets.astype(jnp.float32)


def steps_of(own_key, dims, cuts, low, high):
    loudness, own = 1.0, jax.random.fold_in(own_key, 6)
    for axis_at, blocks in cuts:
        steps = jnp.exp(jax.random.uniform(jax.random.fold_in(own, axis_at), (blocks,), jnp.float32, low / len(cuts), high / len(cuts)))
        loudness = loudness * jnp.repeat(steps, dims[axis_at] // blocks).reshape([-1 if axis == axis_at else 1 for axis in range(len(dims))])
    return loudness


def bell_draw(own_key, shape, deviation, bound, cuts=(), kind=jnp.bfloat16):
    factor_of = steps_of(own_key, shape, cuts, -0.22, 0.18) if cuts else 1.0
    values = jax.random.normal(own_key, shape, jnp.float32) * deviation * factor_of
    return jnp.minimum(jnp.maximum(values, -bound), bound).astype(kind)


def setup_inputs(seed: int = 0, part: int = 0) -> dict:
    key_of = jax.random.split(jax.random.key(seed), 23)
    own_keys = jax.random.split(jax.random.fold_in(key_of[22], part), 23)
    tokens = bell_draw(own_keys[0], (SEQ, MODEL_WIDTH), 1.0, 6.0, ((0, 4), (1, 2)))
    norm_gain = jnp.clip(1.0 + 0.18 * jax.random.normal(key_of[1], (MODEL_WIDTH,), jnp.float32), 0.1, 1.9)
    w_recept = bell_draw(key_of[2], (MODEL_WIDTH, DECAY_CHANNELS), MODEL_WIDTH ** -0.5, 0.125, ((0, 4), (1, 2)))
    w_key_a = bell_draw(key_of[3], (MODEL_WIDTH, DECAY_CHANNELS), MODEL_WIDTH ** -0.5, 0.125, ((0, 4), (1, 2)))
    w_value_a = bell_draw(key_of[4], (MODEL_WIDTH, DECAY_CHANNELS), MODEL_WIDTH ** -0.5, 0.125, ((0, 4), (1, 2)))
    w_gate_a = bell_draw(key_of[5], (MODEL_WIDTH, DECAY_CHANNELS), MODEL_WIDTH ** -0.5, 0.125, ((0, 4), (1, 2)))
    decay_down_weight = bell_draw(key_of[6], (MODEL_WIDTH, LOW_RANK_WIDTH), MODEL_WIDTH ** -0.5, 0.125)
    decay_up_weight = bell_draw(key_of[7], (LOW_RANK_WIDTH, DECAY_CHANNELS), LOW_RANK_WIDTH ** -0.5, 0.75, ((1, 2),))
    rate_down_weight = bell_draw(key_of[8], (MODEL_WIDTH, LOW_RANK_WIDTH), MODEL_WIDTH ** -0.5, 0.125)
    rate_up_weight = bell_draw(key_of[9], (LOW_RANK_WIDTH, DECAY_CHANNELS), LOW_RANK_WIDTH ** -0.5, 0.75, ((1, 2),))
    decay_base = draw_decay_base(jax.random.fold_in(key_of[22], 71), part)
    rate_base = draw_rate_base(jax.random.fold_in(key_of[22], 71), part)
    rate_shift = draw_rate_shift(jax.random.fold_in(jax.random.fold_in(key_of[22], part), 71), part)
    jolts = draw_jolts(jax.random.fold_in(jax.random.fold_in(key_of[22], part), 71), part)
    group_gain = jnp.clip(1.0 + 0.18 * jax.random.normal(key_of[14], (DECAY_CHANNELS,), jnp.float32), 0.1, 1.9)
    w_query_b = bell_draw(key_of[15], (MODEL_WIDTH, WIDTH_B), MODEL_WIDTH ** -0.5, 0.125, ((0, 4), (1, 2)))
    w_key_b = bell_draw(key_of[16], (MODEL_WIDTH, WIDTH_B), MODEL_WIDTH ** -0.5, 0.125, ((0, 4), (1, 2)))
    w_value_b = bell_draw(key_of[17], (MODEL_WIDTH, WIDTH_B), MODEL_WIDTH ** -0.5, 0.125, ((0, 4), (1, 2)))
    w_gate_b = bell_draw(key_of[18], (MODEL_WIDTH, WIDTH_B), MODEL_WIDTH ** -0.5, 0.125, ((0, 4), (1, 2)))
    score_offset = draw_score_offset(jax.random.fold_in(key_of[22], 71), part)
    w_out_a = bell_draw(key_of[20], (DECAY_CHANNELS, MODEL_WIDTH), (DECAY_CHANNELS + WIDTH_B) ** -0.5, 0.125, ((0, 2),))
    w_out_b = bell_draw(key_of[21], (WIDTH_B, MODEL_WIDTH), (DECAY_CHANNELS + WIDTH_B) ** -0.5, 0.125, ((0, 2),))
    return dict(tokens=tokens, norm_gain=norm_gain, w_recept=w_recept, w_key_a=w_key_a, w_value_a=w_value_a, w_gate_a=w_gate_a, decay_down_weight=decay_down_weight, decay_up_weight=decay_up_weight, rate_down_weight=rate_down_weight, rate_up_weight=rate_up_weight, decay_base=decay_base, rate_base=rate_base, rate_shift=rate_shift, jolts=jolts, group_gain=group_gain, w_query_b=w_query_b, w_key_b=w_key_b, w_value_b=w_value_b, w_gate_b=w_gate_b, score_offset=score_offset, w_out_a=w_out_a, w_out_b=w_out_b)


highest = lax.Precision.HIGHEST

def project(normed, matrix):
    return jnp.dot(normed, matrix, preferred_element_type=jnp.float32).astype(jnp.bfloat16)

def decay_step(current, inputs):
    recept_t, decay_t, keys_t, values_t, unit_t, mixing_t = inputs
    removed = jnp.einsum('hvk,hk->hv', current, unit_t, precision=highest)
    current = current * decay_t[:, None, :] - removed[:, :, None] * (unit_t * mixing_t)[:, None, :] + values_t[:, :, None] * keys_t[:, None, :]
    return (current, jnp.einsum('hvk,hk->hv', current, recept_t, precision=highest))

def reference(tokens, norm_gain, w_recept, w_key_a, w_value_a, w_gate_a, decay_down_weight, decay_up_weight, rate_down_weight, rate_up_weight, decay_base, rate_base, rate_shift, jolts, group_gain, w_query_b, w_key_b, w_value_b, w_gate_b, score_offset, w_out_a, w_out_b):
    floats = tokens.astype(jnp.float32)
    normed = (floats * lax.rsqrt(lax.optimization_barrier(jnp.mean(floats * floats, axis=1, keepdims=True)) + 1e-06) * norm_gain).astype(jnp.bfloat16)
    matrices = (w_recept, w_key_a, w_value_a, w_gate_a, w_query_b, w_key_b, w_value_b, w_gate_b)
    recept, keys_a, values_a, gate_a, query_b, keys_b, values_b, gate_b = [project(normed, matrix) for matrix in matrices]
    decay_low = jnp.tanh(jnp.dot(normed, decay_down_weight, preferred_element_type=jnp.float32)).astype(jnp.bfloat16)
    rate_low = project(normed, rate_down_weight)
    preact = decay_base + jnp.dot(decay_low, decay_up_weight, preferred_element_type=jnp.float32) + jnp.repeat(rate_shift, HEAD_A, axis=1)
    decays = jnp.exp(-jnp.exp(-jax.nn.softplus(-preact) - 0.5) - jnp.repeat(jolts, HEAD_A, axis=1))
    mixing = jax.nn.sigmoid(rate_base + jnp.dot(rate_low, rate_up_weight, preferred_element_type=jnp.float32))

    def split_heads(matrix):
        return matrix.astype(jnp.float32).reshape(SEQ, HEADS_A, HEAD_A)
    keys_heads = split_heads(keys_a)
    unit_keys = keys_heads * lax.rsqrt(lax.optimization_barrier(jnp.sum(keys_heads * keys_heads, axis=2, keepdims=True)) + 1e-06)
    start_state = jnp.zeros((HEADS_A, HEAD_A, HEAD_A), jnp.float32)
    inputs = (split_heads(recept), split_heads(decays), keys_heads, split_heads(values_a), unit_keys, split_heads(mixing))
    ignored, reads = lax.scan(decay_step, start_state, inputs)
    centered = reads - lax.optimization_barrier(jnp.mean(reads, axis=2, keepdims=True))
    normal_a = centered * lax.rsqrt(lax.optimization_barrier(jnp.mean(centered * centered, axis=2, keepdims=True)) + 0.00064)
    mixed_a = (normal_a.reshape(SEQ, DECAY_CHANNELS) * group_gain * jax.nn.silu(gate_a.astype(jnp.float32))).astype(jnp.bfloat16)
    factor = HEAD_B ** (-0.5)
    key_place = jnp.arange(SEQ, dtype=jnp.int32)
    rows_here = jnp.arange(TOK_DEV, dtype=jnp.int32)

    def stick_block(block_index):
        head_index = block_index // N_SP
        first_row = (block_index % N_SP * TOK_DEV).astype(jnp.int32)
        column = (head_index * HEAD_B).astype(jnp.int32)
        anchor = jnp.zeros((), jnp.int32)
        queries = lax.dynamic_slice(query_b, (first_row, column), (TOK_DEV, HEAD_B))
        keys_all = lax.dynamic_slice(keys_b, (anchor, column), (SEQ, HEAD_B))
        values_all = lax.dynamic_slice(values_b, (anchor, column), (SEQ, HEAD_B))
        offset = lax.dynamic_index_in_dim(score_offset, head_index, 0, False)
        scores = jnp.dot(queries, keys_all.T, preferred_element_type=jnp.float32) * factor + offset
        causal = key_place[None, :] < (first_row + rows_here)[:, None]
        keep_log = jnp.where(causal, jax.nn.log_sigmoid(-scores), 0.0)
        later_sum = jnp.cumsum(keep_log[:, ::-1], axis=1)[:, ::-1] - keep_log
        weights = jnp.where(causal, jnp.exp(jax.nn.log_sigmoid(scores) + later_sum), 0.0)
        attended = jnp.dot(weights.astype(jnp.bfloat16), values_all, preferred_element_type=jnp.float32)
        return (attended, lax.optimization_barrier(jnp.sum(weights, axis=1)))
    attended, weight_sum = lax.map(stick_block, jnp.arange(HEADS_B * N_SP, dtype=jnp.int32))
    attended = jnp.transpose(attended.reshape(HEADS_B, SEQ, HEAD_B), (1, 0, 2)).reshape(SEQ, WIDTH_B)
    weight_sum = weight_sum.reshape(HEADS_B, SEQ).T
    mixed_b = (attended * jax.nn.silu(gate_b.astype(jnp.float32))).astype(jnp.bfloat16)
    share_a = DECAY_CHANNELS // N_TP
    share_b = WIDTH_B // N_TP
    summed = jnp.zeros((SEQ, MODEL_WIDTH), jnp.float32)
    for group_index in range(N_TP):
        lower_a = group_index * share_a
        lower_b = group_index * share_b
        partial_value = jnp.dot(mixed_a[:, lower_a:lower_a + share_a], w_out_a[lower_a:lower_a + share_a], preferred_element_type=jnp.float32)
        partial_value = partial_value + jnp.dot(mixed_b[:, lower_b:lower_b + share_b], w_out_b[lower_b:lower_b + share_b], preferred_element_type=jnp.float32)
        partial_value = lax.optimization_barrier(partial_value.astype(jnp.bfloat16))
        summed = summed + partial_value.astype(jnp.float32)
    return (summed.astype(jnp.bfloat16), jnp.log(jnp.maximum(weight_sum, 0.01)))
```

```python
import jax
import jax.numpy as jnp
from jax import lax
from jax.experimental import pallas as pl
from jax.experimental.pallas import tpu as pltpu
from jax.sharding import PartitionSpec as P

HEAD_A = 64
HEAD_B = 128


highest = lax.Precision.HIGHEST


def entering_2(value, axis, combine, identity):
    devices, index = (lax.axis_size(axis), lax.axis_index(axis))
    everything = jax.tree.map(
        lambda part, kind: lax.all_gather(part.astype(kind), axis),
        value,
        (jnp.bfloat16, jnp.bfloat16),
    )
    start = jax.tree.map(
        lambda part, zero: jnp.broadcast_to(jnp.asarray(zero, part.dtype), part.shape),
        value,
        identity,
    )

    def lap(k, before):
        reached = k < index
        new = combine(
            before, jax.tree.map(lambda part, own: part[k].astype(own.dtype), everything, value)
        )
        return jax.tree.map(lambda a, b: jnp.where(reached, a, b), new, before)

    return lax.fori_loop(0, devices, lap, start)


def combine_states(earlier, follower):
    joined = jnp.einsum("hij,hjk->hik", earlier[0], follower[0], precision=highest)
    carried = jnp.einsum("hij,hjk->hik", earlier[1], follower[0], precision=highest) + follower[1]
    return (joined, carried)


def block_pass(stacked, pieces):
    recept_c, logs_step, keys_c, values_c, unit_c, mixing_c = pieces
    block_len = recept_c.shape[0]
    totals = jnp.cumsum(logs_step, axis=0)
    preceding = jnp.concatenate([jnp.zeros_like(totals[:1]), totals[:-1]], axis=0)
    steering = unit_c * mixing_c
    places_here = jnp.arange(block_len, dtype=jnp.int32)
    below_diag = (places_here[:, None] > places_here[None, :])[:, :, None, None]
    fading = jnp.where(
        below_diag, jnp.exp(jnp.where(below_diag, preceding[:, None] - totals[None, :], 0.0)), 0.0
    )
    unit_fade = fading * unit_c[:, None]
    weigh_keys = jnp.einsum("tjhc,jhc->htj", unit_fade, keys_c, precision=highest)
    weigh_steer = jnp.einsum("tjhc,jhc->htj", unit_fade, steering, precision=highest)
    read_fade = fading * (recept_c * jnp.exp(logs_step))[:, None]
    diagonal = jnp.eye(block_len, dtype=jnp.float32)
    read_keys = (
        jnp.einsum("tjhc,jhc->htj", read_fade, keys_c, precision=highest)
        + diagonal * jnp.sum(recept_c * keys_c, axis=2).T[:, :, None]
    )
    read_steer = (
        jnp.einsum("tjhc,jhc->htj", read_fade, steering, precision=highest)
        + diagonal * jnp.sum(recept_c * steering, axis=2).T[:, :, None]
    )
    values_wide = jnp.concatenate([jnp.zeros_like(values_c), values_c], axis=2)
    entering = jnp.einsum("thc,hrc->htr", unit_c * jnp.exp(preceding), stacked, precision=highest)
    entering = entering + jnp.einsum("htj,jhr->htr", weigh_keys, values_wide, precision=highest)
    removal = jax.scipy.linalg.solve_triangular(
        weigh_steer + diagonal, entering, lower=True, unit_diagonal=True
    )
    readout = jnp.einsum("thc,hrc->htr", recept_c * jnp.exp(totals), stacked, precision=highest)
    readout = readout + jnp.einsum("htj,jhr->htr", read_keys, values_wide, precision=highest)
    readout = readout - jnp.einsum("htj,hjr->htr", read_steer, removal, precision=highest)
    tail_fade = jnp.exp(totals[-1][None] - totals)
    closing = stacked * jnp.exp(totals[-1])[:, None, :]
    closing = closing + jnp.einsum(
        "jhr,jhc->hrc", values_wide, keys_c * tail_fade, precision=highest
    )
    closing = closing - jnp.einsum("hjr,jhc->hrc", removal, steering * tail_fade, precision=highest)
    return (closing, jnp.transpose(readout, (1, 0, 2)))


def local_positions(
    tokens,
    norm_gain,
    w_recept,
    w_key_a,
    w_value_a,
    w_gate_a,
    decay_down_weight,
    decay_up_weight,
    rate_down_weight,
    rate_up_weight,
    decay_base,
    rate_base,
    rate_shift,
    jolts,
    group_gain,
    w_query_b,
    w_key_b,
    w_value_b,
    w_gate_b,
    score_offset,
    w_out_a,
    w_out_b,
):
    gathered = lax.all_gather(tokens, "tp", axis=1, tiled=True)
    floats = gathered.astype(jnp.float32)
    normed = (
        floats * lax.rsqrt(jnp.mean(floats * floats, axis=1, keepdims=True) + 1e-06) * norm_gain
    ).astype(jnp.bfloat16)
    row_count = normed.shape[0]
    matrices = (w_recept, w_key_a, w_value_a, w_gate_a, w_query_b, w_key_b, w_value_b, w_gate_b)
    portions = (
        lax.all_gather(matrices[0], "sp", axis=0, tiled=True),
        lax.all_gather(matrices[1], "sp", axis=0, tiled=True),
        lax.all_gather(matrices[2], "sp", axis=0, tiled=True),
        lax.all_gather(matrices[3], "sp", axis=0, tiled=True),
        lax.all_gather(matrices[4], "sp", axis=0, tiled=True),
        lax.all_gather(matrices[5], "sp", axis=0, tiled=True),
        lax.all_gather(matrices[6], "sp", axis=0, tiled=True),
        lax.all_gather(matrices[7], "sp", axis=0, tiled=True),
    )
    projected = tuple(
        (jnp.dot(normed, portion, preferred_element_type=jnp.float32) for portion in portions)
    )
    recept, keys_a, values_a, gate_a, query_b, keys_b, values_b, gate_b = [
        summed.astype(jnp.bfloat16) for summed in projected
    ]
    heads_a = recept.shape[1] // HEAD_A
    decay_low = jnp.tanh(
        jnp.dot(normed, decay_down_weight, preferred_element_type=jnp.float32)
    ).astype(jnp.bfloat16)
    rate_low = jnp.dot(normed, rate_down_weight, preferred_element_type=jnp.float32).astype(
        jnp.bfloat16
    )
    preact = (
        decay_base
        + jnp.dot(decay_low, decay_up_weight, preferred_element_type=jnp.float32)
        + jnp.repeat(rate_shift, HEAD_A, axis=1)
    )
    log_decay = -jnp.exp(-jax.nn.softplus(-preact) - 0.5) - jnp.repeat(jolts, HEAD_A, axis=1)
    mixing = jax.nn.sigmoid(
        rate_base + jnp.dot(rate_low, rate_up_weight, preferred_element_type=jnp.float32)
    )

    def split_heads(matrix):
        return matrix.astype(jnp.float32).reshape(row_count, heads_a, HEAD_A)

    keys_heads = split_heads(keys_a)
    unit_keys = keys_heads * lax.rsqrt(
        jnp.sum(keys_heads * keys_heads, axis=2, keepdims=True) + 1e-06
    )
    block_len = min(32, row_count)
    block_count = row_count // block_len

    def to_blocks(matrix):
        return matrix.reshape(block_count, block_len, heads_a, HEAD_A)

    inputs = tuple(
        (
            to_blocks(matrix)
            for matrix in (
                split_heads(recept),
                log_decay.reshape(row_count, heads_a, HEAD_A),
                keys_heads,
                split_heads(values_a),
                unit_keys,
                mixing.reshape(row_count, heads_a, HEAD_A),
            )
        )
    )
    identity = jnp.broadcast_to(jnp.eye(HEAD_A, dtype=jnp.float32), (heads_a, HEAD_A, HEAD_A))
    zeros_state = jnp.zeros((heads_a, HEAD_A, HEAD_A), jnp.float32)
    closing, readout = lax.scan(
        block_pass, jnp.concatenate([identity, zeros_state], axis=1), inputs
    )
    readout = readout.reshape(row_count, heads_a, 2 * HEAD_A)
    prefix = entering_2(
        (closing[:, :HEAD_A], closing[:, HEAD_A:]), "sp", combine_states, (identity, zeros_state)
    )
    outputs_a = readout[:, :, HEAD_A:] + jnp.einsum(
        "hvk,thk->thv", prefix[1], readout[:, :, :HEAD_A], precision=highest
    )
    centered = outputs_a - jnp.mean(outputs_a, axis=2, keepdims=True)
    normal_a = centered * lax.rsqrt(jnp.mean(centered * centered, axis=2, keepdims=True) + 0.00064)
    mixed_a = (
        normal_a.reshape(row_count, -1) * group_gain * jax.nn.silu(gate_a.astype(jnp.float32))
    ).astype(jnp.bfloat16)
    heads_b = query_b.shape[1] // HEAD_B
    own_index = lax.axis_index("sp")
    places = jnp.arange(row_count, dtype=jnp.int32)
    query_place = own_index * row_count + places
    query_heads = query_b.reshape(row_count, heads_b, HEAD_B)
    factor = HEAD_B ** (-0.5)
    paired = jnp.stack(
        [keys_b.reshape(row_count, heads_b, HEAD_B), values_b.reshape(row_count, heads_b, HEAD_B)]
    )

    def attend(running, paired_piece, source):
        attended, weight_sum, survive = running
        scores = (
            jnp.einsum(
                "qhd,khd->hqk", query_heads, paired_piece[0], preferred_element_type=jnp.float32
            )
            * factor
            + score_offset[:, None, None]
        )
        causal = (source * row_count + places)[None, None, :] < query_place[None, :, None]
        keep_log = jnp.where(causal, jax.nn.log_sigmoid(-scores), 0.0)
        later_sum = (
            jnp.flip(jnp.cumsum(jnp.flip(keep_log, 2), axis=2), 2) - keep_log + survive[:, :, None]
        )
        weights = jnp.where(causal, jnp.exp(jax.nn.log_sigmoid(scores) + later_sum), 0.0)
        attended = attended + jnp.einsum(
            "hqk,khd->qhd",
            weights.astype(jnp.bfloat16),
            paired_piece[1],
            preferred_element_type=jnp.float32,
        )
        return (
            attended,
            weight_sum + jnp.sum(weights, axis=2),
            survive + jnp.sum(keep_log, axis=2),
        )

    empty_b = (
        jnp.zeros((row_count, heads_b, HEAD_B), jnp.float32),
        jnp.zeros((heads_b, row_count), jnp.float32),
        jnp.zeros((heads_b, row_count), jnp.float32),
    )
    running = attend(empty_b, paired, own_index)
    all_pairs = lax.all_gather(paired[None], "sp", axis=0, tiled=True)

    def visit_piece(rounds, holding):
        source = own_index - rounds
        chosen = lax.dynamic_index_in_dim(all_pairs, jnp.maximum(source, 0), 0, False)
        return lax.cond(
            source >= 0, lambda kept: attend(kept, chosen, source), lambda kept: kept, holding
        )

    running = lax.fori_loop(1, lax.axis_size("sp"), visit_piece, running)
    mixed_b = (running[0].reshape(row_count, -1) * jax.nn.silu(gate_b.astype(jnp.float32))).astype(
        jnp.bfloat16
    )
    row_log = jnp.log(jnp.maximum(running[1].T, 0.01))
    mixed = lax.psum_scatter(
        (
            jnp.dot(mixed_a, w_out_a, preferred_element_type=jnp.float32)
            + jnp.dot(mixed_b, w_out_b, preferred_element_type=jnp.float32)
        ).astype(jnp.bfloat16),
        "tp",
        scatter_dimension=0,
        tiled=True,
    )
    return (mixed, row_log)


LANES = 128
CHUNK = 64
TOGETHER = 4


def dot_t(a, b, dims):
    return lax.dot_general(a, b, (dims, ((), ())), preferred_element_type=jnp.float32)


def split(a):
    high = a.astype(jnp.bfloat16)
    return high, (a - high.astype(jnp.float32)).astype(jnp.bfloat16)


def mm(a, b, dims=((1,), (0,))):
    a_high, a_low = split(a)
    b_high, b_low = split(b)
    return dot_t(a_high, b_high, dims) + (dot_t(a_high, b_low, dims) + dot_t(a_low, b_high, dims))


NT = ((1,), (1,))
TN = ((0,), (0,))


def project_kernel(x_ref, *refs):
    weights, out_ref = refs[:-1], refs[-1]
    x = x_ref[...]
    for i, w_ref in enumerate(weights):
        result = jnp.dot(x, w_ref[...], preferred_element_type=jnp.float32).astype(jnp.bfloat16)
        for s in range(out_ref.shape[0]):
            out_ref[s, :, i * LANES : (i + 1) * LANES] = result[:, s * LANES : (s + 1) * LANES]


def project(x, weights, shares):
    return pl.pallas_call(
        project_kernel,
        out_shape=jax.ShapeDtypeStruct((shares, x.shape[0], LANES * len(weights)), jnp.bfloat16),
    )(x, *weights)


def per_head_sum(a, first):
    left = jnp.sum(jnp.where(first, a, 0.0), axis=1, keepdims=True)
    right = jnp.sum(jnp.where(first, 0.0, a), axis=1, keepdims=True)
    return jnp.where(first, left, right)


def state_kernel(
    rkv_ref, low_ref, up_ref, vec_ref, out_ref, m_ref, b_ref, p_ref, n_ref, log_ref, mix_ref, unit_ref
):
    rows = rkv_ref.shape[0]
    first = lax.broadcasted_iota(jnp.int32, (1, LANES), 1) < HEAD_A
    low = low_ref[...]
    rank = up_ref.shape[0] // 2
    decay_low = low[:, :rank].astype(jnp.bfloat16)
    rate_low = low[:, rank : 2 * rank].astype(jnp.bfloat16)
    extra = low[:, 2 * rank :]
    shift = jnp.where(first, extra[:, 0:1], extra[:, 1:2])
    jolt = jnp.where(first, extra[:, 2:3], extra[:, 3:4])
    preact = vec_ref[0:1] + jnp.dot(decay_low, up_ref[:rank], preferred_element_type=jnp.float32) + shift
    log_ref[...] = -jnp.exp(-0.5) * jax.nn.sigmoid(preact) - jolt
    mix_ref[...] = jax.nn.sigmoid(
        vec_ref[1:2] + jnp.dot(rate_low, up_ref[rank:], preferred_element_type=jnp.float32)
    )
    keys_all = rkv_ref[:, LANES : 2 * LANES].astype(jnp.float32)
    unit_ref[...] = keys_all * lax.rsqrt(per_head_sum(keys_all * keys_all, first) + 1e-06)

    row = lax.broadcasted_iota(jnp.int32, (LANES, LANES), 0)
    col = lax.broadcasted_iota(jnp.int32, (LANES, LANES), 1)
    same_head = (row // CHUNK) == (col // CHUNK)
    strict = same_head & (row > col)
    inclusive = same_head & (row >= col)
    eye = (row == col).astype(jnp.float32)
    tri = (
        lax.broadcasted_iota(jnp.int32, (CHUNK, CHUNK), 0)
        >= lax.broadcasted_iota(jnp.int32, (CHUNK, CHUNK), 1)
    ).astype(jnp.bfloat16)

    def stack(a):
        return jnp.concatenate([jnp.where(first, a, 0.0), jnp.where(first, 0.0, a)], axis=0)

    def inverse(lower):
        near = (row // 16) == (col // 16)
        power = jnp.where(near, lower, 0.0)
        result = eye - power
        for _ in range(3):
            power = mm(power, power)
            result = result + mm(result, power)
        size = 16
        while size < CHUNK:
            joining = (row // size != col // size) & (row // (2 * size) == col // (2 * size))
            corner = jnp.where(joining, lower, 0.0)
            result = result - mm(mm(result, corner), result)
            size = 2 * size
        return result

    def prepare(c):
        at = pl.ds(pl.multiple_of(c * CHUNK, CHUNK), CHUNK)
        logs = log_ref[at]
        log_high, log_low = split(logs)
        log_last = (logs - log_high.astype(jnp.float32) - log_low.astype(jnp.float32)).astype(jnp.bfloat16)
        dims = ((1,), (0,))
        totals = dot_t(tri, log_high, dims) + (dot_t(tri, log_low, dims) + dot_t(tri, log_last, dims))
        preceding = totals - logs
        middle = totals[CHUNK // 2 - 1 : CHUNK // 2]
        final = totals[CHUNK - 1 : CHUNK]
        recept = rkv_ref[at, 0:LANES].astype(jnp.float32)
        keys = rkv_ref[at, LANES : 2 * LANES].astype(jnp.float32)
        values = stack(rkv_ref[at, 2 * LANES : 3 * LANES].astype(jnp.float32))
        unit = unit_ref[at]
        steer = unit * mix_ref[at]
        growth = jnp.exp(middle - totals)
        unit_in = stack(unit * jnp.exp(preceding - middle))
        recept_in = stack(recept * jnp.exp(totals - middle))
        keys_out = stack(keys * growth)
        steer_out = stack(steer * growth)
        weigh_keys = jnp.where(strict, mm(unit_in, keys_out, NT), 0.0)
        weigh_steer = jnp.where(strict, mm(unit_in, steer_out, NT), 0.0)
        read_keys = jnp.where(inclusive, mm(recept_in, keys_out, NT), 0.0)
        read_steer = jnp.where(inclusive, mm(recept_in, steer_out, NT), 0.0)
        solved = inverse(weigh_steer)
        fade = jnp.exp(final - totals)
        keys_end = stack(keys * fade)
        steer_end = stack(steer * fade)
        q = mm(solved, stack(unit * jnp.exp(preceding)))
        u = mm(solved, mm(weigh_keys, values))
        m_ref[c] = eye * jnp.exp(final) - mm(steer_end, q, TN)
        b_ref[c] = mm(keys_end, values, TN) - mm(steer_end, u, TN)
        p_ref[c] = stack(recept * jnp.exp(totals)) - mm(read_steer, q)
        n_ref[c] = mm(read_keys, values) - mm(read_steer, u)

    chunks = rows // CHUNK
    together = TOGETHER if chunks % TOGETHER == 0 else 1

    def lap(i, nothing):
        for k in range(together):
            prepare(i * together + k)
        return nothing

    lax.fori_loop(0, chunks // together, lap, 0)

    def advance(c, state):
        reads = mm(p_ref[c], state) + n_ref[c]
        out_ref[pl.ds(pl.multiple_of(c * CHUNK, CHUNK), CHUNK), :] = reads[:CHUNK] + reads[CHUNK:]
        return mm(m_ref[c], state) + b_ref[c]

    lax.fori_loop(0, chunks, advance, jnp.zeros((LANES, LANES), jnp.float32))
    reads = out_ref[...]
    centered = reads - per_head_sum(reads, first) * (1.0 / HEAD_A)
    variance = per_head_sum(centered * centered, first) * (1.0 / HEAD_A)
    out_ref[...] = centered * lax.rsqrt(variance + 0.00064) * vec_ref[2:3]


def state_mixer(rkv, low, up, vectors):
    rows = rkv.shape[0]
    square = pltpu.VMEM((rows // CHUNK, LANES, LANES), jnp.float32)
    full = pltpu.VMEM((rows, LANES), jnp.float32)
    return pl.pallas_call(
        state_kernel,
        out_shape=jax.ShapeDtypeStruct((rows, LANES), jnp.float32),
        scratch_shapes=[square, square, square, square, full, full, full],
    )(rkv, low, up, vectors)


def silu(a):
    return a * jax.nn.sigmoid(a)


def stick_kernel(rest_ref, normal_ref, offset_ref, out_ref):
    rows = rest_ref.shape[0]
    factor = HEAD_B ** (-0.5)
    row = lax.broadcasted_iota(jnp.int32, (LANES, LANES), 0)
    col = lax.broadcasted_iota(jnp.int32, (LANES, LANES), 1)
    causal = col < row
    later = (row > col).astype(jnp.bfloat16)
    gate_a = rest_ref[:, 3 * LANES : 4 * LANES].astype(jnp.float32)
    out_ref[:, 0:LANES] = (normal_ref[...] * silu(gate_a)).astype(jnp.bfloat16)
    offset = offset_ref[0:1, :]
    dims = ((1,), (0,))
    for i in range(rows // LANES):
        at = slice(i * LANES, (i + 1) * LANES)
        query = rest_ref[at, 0:LANES]
        survive = jnp.zeros((LANES, 1), jnp.float32)
        weight_sum = jnp.zeros((LANES, 1), jnp.float32)
        attended = jnp.zeros((LANES, LANES), jnp.float32)
        for j in range(i, -1, -1):
            there = slice(j * LANES, (j + 1) * LANES)
            scores = dot_t(query, rest_ref[there, LANES : 2 * LANES], NT) * factor + offset
            keep = -(jnp.maximum(scores, 0.0) + jnp.log1p(jnp.exp(-jnp.abs(scores))))
            taken = scores + keep
            if i == j:
                keep = jnp.where(causal, keep, 0.0)
            keep_high, keep_low = split(keep)
            after = dot_t(keep_high, later, dims) + dot_t(keep_low, later, dims)
            weights = jnp.exp(taken + after + survive)
            if i == j:
                weights = jnp.where(causal, weights, 0.0)
            survive = survive + jnp.sum(keep, axis=1, keepdims=True)
            weight_sum = weight_sum + jnp.sum(weights, axis=1, keepdims=True)
            attended = attended + dot_t(
                weights.astype(jnp.bfloat16), rest_ref[there, 2 * LANES : 3 * LANES], dims
            )
        gate_b = rest_ref[at, 4 * LANES : 5 * LANES].astype(jnp.float32)
        out_ref[at, LANES : 2 * LANES] = (attended * silu(gate_b)).astype(jnp.bfloat16)
        row_log = jnp.log(jnp.maximum(weight_sum, 0.01))
        log_high = row_log.astype(jnp.bfloat16).astype(jnp.float32)
        log_low = (row_log - log_high).astype(jnp.bfloat16).astype(jnp.float32)
        out_ref[at, 2 * LANES : 3 * LANES] = jnp.where(
            col == 0, log_high, jnp.where(col == 1, log_low, 0.0)
        ).astype(jnp.bfloat16)


def stick_mixer(rest, normal, offset):
    return pl.pallas_call(
        stick_kernel,
        out_shape=jax.ShapeDtypeStruct((rest.shape[0], 3 * LANES), jnp.bfloat16),
    )(rest, normal, offset)


def local_heads(
    tokens,
    norm_gain,
    w_recept,
    w_key_a,
    w_value_a,
    w_gate_a,
    decay_down_weight,
    decay_up_weight,
    rate_down_weight,
    rate_up_weight,
    decay_base,
    rate_base,
    rate_shift,
    jolts,
    group_gain,
    w_query_b,
    w_key_b,
    w_value_b,
    w_gate_b,
    score_offset,
    w_out_a,
    w_out_b,
):
    shares, index = lax.axis_size("sp"), lax.axis_index("sp")
    gathered = lax.all_gather(tokens, "tp", axis=1, tiled=True)
    floats = gathered.astype(jnp.float32)
    normed = (
        floats * lax.rsqrt(jnp.mean(floats * floats, axis=1, keepdims=True) + 1e-06) * norm_gain
    ).astype(jnp.bfloat16)
    rows = normed.shape[0]
    features = lax.all_to_all(normed, "sp", split_axis=1, concat_axis=0, tiled=True)
    decay_low = jnp.tanh(jnp.dot(normed, decay_down_weight, preferred_element_type=jnp.float32))
    rate_low = jnp.dot(normed, rate_down_weight, preferred_element_type=jnp.float32)
    small = jnp.concatenate([decay_low, rate_low, rate_shift, jolts], axis=1)
    small = lax.all_gather(small, "sp", axis=0, tiled=True)
    rank = decay_low.shape[1]
    local_a = rate_shift.shape[1]
    own_a = local_a // shares

    def own(array, size, start=0):
        return lax.dynamic_slice_in_dim(array, start + index * size, size, axis=array.ndim - 1)

    low = jnp.concatenate(
        [
            small[:, : 2 * rank],
            own(small, own_a, 2 * rank),
            own(small, own_a, 2 * rank + local_a),
        ],
        axis=1,
    )
    up = own(jnp.concatenate([decay_up_weight, rate_up_weight], axis=0), LANES)
    vectors = own(jnp.stack([decay_base, rate_base, group_gain]), LANES)
    offset = jnp.broadcast_to(own(score_offset, score_offset.shape[0] // shares), (8, LANES))

    part_a = project(features, (w_recept, w_key_a, w_value_a), shares)
    rkv = lax.psum_scatter(part_a, "sp", scatter_dimension=0, tiled=True)[0]
    part_b = project(features, (w_query_b, w_key_b, w_value_b, w_gate_a, w_gate_b), shares)
    rest = lax.psum_scatter(part_b, "sp", scatter_dimension=0, tiled=True)[0]
    normal = state_mixer(rkv, low, up, vectors)
    both = stick_mixer(rest, normal, offset)
    back = lax.all_to_all(
        both.reshape(shares, rows, 3 * LANES), "sp", split_axis=0, concat_axis=0, tiled=True
    )
    back = jnp.transpose(back, (1, 0, 2))
    mixed_a = back[:, :, :LANES].reshape(rows, -1)
    mixed_b = back[:, :, LANES : 2 * LANES].reshape(rows, -1)
    logs = back[:, :, 2 * LANES : 2 * LANES + 2].astype(jnp.float32)
    row_log = logs[:, :, 0] + logs[:, :, 1]
    mixed = lax.psum_scatter(
        (
            jnp.dot(mixed_a, w_out_a, preferred_element_type=jnp.float32)
            + jnp.dot(mixed_b, w_out_b, preferred_element_type=jnp.float32)
        ).astype(jnp.bfloat16),
        "tp",
        scatter_dimension=0,
        tiled=True,
    )
    return (mixed, row_log)


def solution(mesh):
    def chosen(*arrays):
        width = arrays[2].shape[1]
        shares = mesh.shape["sp"]
        whole_heads = width == shares * LANES and arrays[15].shape[1] == width
        rows = arrays[0].shape[0]
        if whole_heads and rows % LANES == 0:
            return local_heads(*arrays)
        return local_positions(*arrays)

    in_specs = (
        P(("fs", "sp"), "tp"),
        P(),
        P("sp", "tp"),
        P("sp", "tp"),
        P("sp", "tp"),
        P("sp", "tp"),
        P(),
        P(None, "tp"),
        P(),
        P(None, "tp"),
        P("tp"),
        P("tp"),
        P(("fs", "sp"), "tp"),
        P(("fs", "sp"), "tp"),
        P("tp"),
        P("sp", "tp"),
        P("sp", "tp"),
        P("sp", "tp"),
        P("sp", "tp"),
        P("tp"),
        P("tp", None),
        P("tp", None),
    )
    out_specs = (P(("fs", "sp", "tp"), None), P(("fs", "sp"), "tp"))
    return jax.shard_map(chosen, mesh=mesh, in_specs=in_specs, out_specs=out_specs, check_vma=False)
```
